32 devices in a mesh: grp: 2 (over y), fs: 4 (over z), tp: 4 (over x, core).
Axes of the slice: x: 2, y: 2, z: 4, core: 2. Of those that a mesh axis runs over, the one named last changes fastest.
Arguments:
- tokens: bfloat16 [2560, 2048], P(('grp', 'fs', 'tp')), parts along dimension 0, may hold values from -6 to 6
- mix_gain: bfloat16 [2048], replicated, may hold values from 0.099609375 to 1.8984375
- val_weight: bfloat16 [2048, 1024], P('fs', 'tp'), may hold values from -4 to 4
- gate_weight: bfloat16 [2048, 1024], P('fs', 'tp'), may hold values from -0.125 to 0.125
- conv_taps: bfloat16 [31, 1024], replicated, may hold values from -1 to 1
- chan_gain: bfloat16 [1024], replicated, may hold values from 0.099609375 to 1.8984375
- out_weight: bfloat16 [1024, 2048], P('tp', 'fs'), may hold values from -0.1875 to 0.1875
- mix_post_gain: bfloat16 [2048], replicated, may hold values from 0.099609375 to 1.8984375
- ffn_gain: bfloat16 [2048], replicated, may hold values from 0.099609375 to 1.8984375
- up_gate_weight: bfloat16 [2048, 5120], P('fs', 'tp'), may hold values from -0.125 to 0.125
- up_val_weight: bfloat16 [2048, 5120], P('fs', 'tp'), may hold values from -0.125 to 0.125
- ffn_taps: bfloat16 [2, 3, 5120], replicated, may hold values from -3.5 to 3.5
- down_weight: bfloat16 [5120, 2048], P('tp', 'fs'), may hold values from -0.078125 to 0.078125
- ffn_post_gain: bfloat16 [2048], replicated, may hold values from 0.099609375 to 1.8984375
Outputs:
- layer_out: bfloat16 [2560, 2048], P(('grp', 'fs', 'tp')), parts along dimension 0
The draws below stay inside these ranges and needn't reach their ends.
There are 2 independent parts, one for each index of `grp`. The reference program is written for one: setup_inputs(seed, part) draws one part's arguments, and reference() takes and returns one part's arrays. A program takes and returns all parts, laid end to end along the dimension named above; an argument that names none is the same for every part. Nothing has to cross between parts.
All inputs are finite; a program needn't handle non-finite values.
Results may differ from the reference program's by a relative error of at most 0.019.
Values may be sent and summed in bfloat16 or wider, within the bound.
A program may use at most 64 MiB of HBM per device.

```python
import jax
import jax.numpy as jnp
from jax import lax

D = 2048
CH = 1024
FF = 5120
CONV_TAPS = 31
FFN_TAPS = 3
LEN = 64
TOKENS = 1280
N_TP = 4


def draw_val_weight(key, part):
    base_key, rough_key = jax.random.split(key, 2)
    base_draw = jax.random.normal(base_key, (D, CH), jnp.float32) * D ** (-0.5)
    roughness = jnp.exp(jax.random.uniform(rough_key, (CH,), jnp.float32, -0.7, 0.7))
    position = jnp.arange(CH, dtype=jnp.float32) / CH
    drawn_values = base_draw * 4.0 ** position * roughness
    return jnp.clip(drawn_values, -4.0, 4.0).astype(jnp.bfloat16)


def shard_levels(rng, dims, pieces, smallest, top_value):
    level = 1.0
    for dim, shards_of in pieces:
        steps = jax.random.uniform(jax.random.fold_in(jax.random.fold_in(rng, 6), dim), (shards_of,), jnp.float32, smallest / len(pieces), top_value / len(pieces))
        level = level * jnp.repeat(jnp.exp(steps), dims[dim] // shards_of).reshape((-1,) + (1,) * (len(dims) - 1 - dim))
    return level


def gaussian(rng, shape, scale, most, cuts=(), held_as=jnp.bfloat16):
    values = jax.random.normal(rng, shape, jnp.float32) * scale
    if len(cuts) > 0:
        values = shard_levels(rng, shape, cuts, -0.22, 0.18) * values
    return jnp.clip(values, min=-most, max=most).astype(held_as)


def setup_inputs(seed: int = 0, part: int = 0) -> dict:
    splits = jax.random.split(jax.random.key(seed), 15)
    part_splits = jax.random.split(jax.random.fold_in(splits[14], part), 15)
    return {
        "tokens": gaussian(part_splits[0], (TOKENS, D), 1.0, 6.0, ((0, 16),)),
        "mix_gain": jnp.clip(1.0 + 0.18 * jax.random.normal(splits[1], (D,), jnp.float32), 0.099609375, 1.8984375).astype(jnp.bfloat16),
        "val_weight": draw_val_weight(jax.random.fold_in(splits[14], 71), part),
        "gate_weight": gaussian(splits[3], (D, CH), D ** -0.5, 0.125, ((0, 4), (1, 4))),
        "conv_taps": gaussian(splits[4], (CONV_TAPS, CH), CONV_TAPS ** -0.5, 1.0),
        "chan_gain": jnp.clip(1.0 + 0.18 * jax.random.normal(splits[5], (CH,), jnp.float32), 0.099609375, 1.8984375).astype(jnp.bfloat16),
        "out_weight": gaussian(splits[6], (CH, D), CH ** -0.5, 0.1875, ((0, 4), (1, 4))),
        "mix_post_gain": jnp.clip(1.0 + 0.18 * jax.random.normal(splits[7], (D,), jnp.float32), 0.099609375, 1.8984375).astype(jnp.bfloat16),
        "ffn_gain": jnp.clip(1.0 + 0.18 * jax.random.normal(splits[8], (D,), jnp.float32), 0.099609375, 1.8984375).astype(jnp.bfloat16),
        "up_gate_weight": gaussian(splits[9], (D, FF), D ** -0.5, 0.125, ((0, 4), (1, 4))),
        "up_val_weight": gaussian(splits[10], (D, FF), D ** -0.5, 0.125, ((0, 4), (1, 4))),
        "ffn_taps": gaussian(splits[11], (2, FFN_TAPS, FF), FFN_TAPS ** -0.5, 3.5),
        "down_weight": gaussian(splits[12], (FF, D), FF ** -0.5, 0.078125, ((0, 4), (1, 4))),
        "ffn_post_gain": jnp.clip(1.0 + 0.18 * jax.random.normal(splits[13], (D,), jnp.float32), 0.099609375, 1.8984375).astype(jnp.bfloat16),
    }


norm_epsilon = 1e-06
chan_epsilon = 1e-05

def rms_scale(values, gain):
    inverse = lax.rsqrt(lax.optimization_barrier(jnp.mean(values * values, axis=-1, keepdims=True)) + norm_epsilon)
    return values * inverse * gain.astype(jnp.float32)

def depthwise(signal, tap_table):
    taps_count = tap_table.shape[0]
    channels = signal.shape[1]
    shaped = signal.astype(jnp.float32).reshape(signal.shape[0] // LEN, LEN, channels)
    padded = jnp.pad(shaped, ((0, 0), (taps_count - 1, 0), (0, 0)))
    tap_values = tap_table.astype(jnp.float32)
    result = jnp.zeros(shaped.shape, jnp.float32)
    for offset in range(taps_count):
        result = result + padded[:, offset:offset + LEN, :] * tap_values[offset]
    return result.reshape(signal.shape[0], channels)

def grouped_sum(left, weight):
    group_width = left.shape[1] // N_TP

    def step(running, group_index):
        columns = lax.dynamic_slice_in_dim(left, group_index * group_width, group_width, 1)
        row_block = lax.dynamic_slice_in_dim(weight, group_index * group_width, group_width, 0)
        partial_value = jnp.dot(columns, row_block, preferred_element_type=jnp.float32).astype(jnp.bfloat16)
        partial_value = lax.optimization_barrier(partial_value)
        return (running + partial_value.astype(jnp.float32), None)
    start_sum = jnp.zeros((left.shape[0], weight.shape[1]), jnp.float32)
    running, _ = lax.scan(step, start_sum, jnp.arange(N_TP, dtype=jnp.int32))
    return running

def reference(tokens, mix_gain, val_weight, gate_weight, conv_taps, chan_gain, out_weight, mix_post_gain, ffn_gain, up_gate_weight, up_val_weight, ffn_taps, down_weight, ffn_post_gain):
    normed = rms_scale(tokens.astype(jnp.float32), mix_gain).astype(jnp.bfloat16)
    values = jnp.dot(normed, val_weight, preferred_element_type=jnp.float32)
    gate_sums = jnp.dot(normed, gate_weight, preferred_element_type=jnp.float32)
    glu_out = (values * jax.nn.sigmoid(gate_sums)).astype(jnp.bfloat16)
    conv_out = depthwise(glu_out, conv_taps)
    chan_mean = lax.optimization_barrier(jnp.mean(conv_out, axis=-1, keepdims=True))
    chan_var = lax.optimization_barrier(jnp.mean(conv_out * conv_out, axis=-1, keepdims=True)) - chan_mean * chan_mean
    scaled = (conv_out - chan_mean) * lax.rsqrt(chan_var + chan_epsilon) * chan_gain.astype(jnp.float32)
    activated = jax.nn.silu(scaled).astype(jnp.bfloat16)
    mixed_sum = grouped_sum(activated, out_weight)
    residual = (tokens.astype(jnp.float32) + rms_scale(mixed_sum, mix_post_gain)).astype(jnp.bfloat16)
    normed_ffn = rms_scale(residual.astype(jnp.float32), ffn_gain).astype(jnp.bfloat16)
    up_gate = jnp.dot(normed_ffn, up_gate_weight, preferred_element_type=jnp.float32).astype(jnp.bfloat16)
    up_val = jnp.dot(normed_ffn, up_val_weight, preferred_element_type=jnp.float32).astype(jnp.bfloat16)
    gate_conv = depthwise(up_gate, ffn_taps[0])
    val_conv = depthwise(up_val, ffn_taps[1])
    hidden = (jax.nn.gelu(gate_conv, approximate=True) * val_conv).astype(jnp.bfloat16)
    ffn_sum = grouped_sum(hidden, down_weight)
    return (residual.astype(jnp.float32) + rms_scale(ffn_sum, ffn_post_gain)).astype(jnp.bfloat16)
```

```python
import functools

import jax
import jax.numpy as jnp
from jax import lax
from jax.experimental import pallas as pl
from jax.experimental.pallas import tpu as pltpu
from jax.sharding import PartitionSpec as P

LEN = 64


norm_epsilon = 1e-06
chan_epsilon = 1e-05


def rms_scale(values, gain):
    inverse = lax.rsqrt(jnp.mean(values * values, axis=-1, keepdims=True) + norm_epsilon)
    return values * inverse * gain.astype(jnp.float32)


def depthwise(signal, tap_table):
    taps_count = tap_table.shape[0]
    channels = signal.shape[1]
    shaped = signal.astype(jnp.float32).reshape(signal.shape[0] // LEN, LEN, channels)
    padded = jnp.pad(shaped, ((0, 0), (taps_count - 1, 0), (0, 0)))
    tap_values = tap_table.astype(jnp.float32)
    result = jnp.zeros(shaped.shape, jnp.float32)
    for offset in range(taps_count):
        result = result + padded[:, offset : offset + LEN, :] * tap_values[offset]
    return result.reshape(signal.shape[0], channels)


def make_adder(left, pieces):
    first = jnp.dot(left, pieces[0], preferred_element_type=jnp.float32)
    second = jnp.dot(left, pieces[1], preferred_element_type=jnp.float32)
    return (first, second)


def make_rows_product(left, weight):
    return jnp.dot(left, weight, preferred_element_type=jnp.float32)


class LineGather:
    def __init__(self, count, sources, gathered, semaphores):
        self.count = count
        self.sources = sources
        self.gathered = gathered
        self.z_send, self.z_recv, self.y_send, self.y_recv, self.own_sem = semaphores
        self.place = lax.axis_index("fs")
        self.half = lax.axis_index("grp")

    def barrier(self, extra=()):
        place, count = self.place, self.count
        semaphore = pltpu.get_barrier_semaphore()
        for step in (1, -1):

            @pl.when(self.has(step, 1))
            def _():
                pl.semaphore_signal(semaphore, inc=1, device_id={"fs": place + step})

        others = [{"grp": 1 - self.half}] + list(extra)
        for other in others:
            pl.semaphore_signal(semaphore, inc=1, device_id=other)
        inner = (place > 0).astype(jnp.int32) + (place < count - 1).astype(jnp.int32)
        pl.semaphore_wait(semaphore, inner + len(others))

    def has(self, step, distance):
        if step > 0:
            return self.place + distance < self.count
        return self.place >= distance

    def rows(self, index, half):
        size = self.sources[index].shape[0] // 2
        return pl.ds(pl.multiple_of(half * size, size), size)

    def z_copy(self, index, way, distance):
        step = 1 if way == 0 else -1
        origin = self.place - step * distance
        rows = self.rows(index, self.half)
        target = self.gathered[index].at[origin, rows]
        source = self.sources[index].at[rows] if distance == 0 else target
        return pltpu.make_async_remote_copy(
            src_ref=source,
            dst_ref=target,
            send_sem=self.z_send.at[index, way, distance],
            recv_sem=self.z_recv.at[index, way, distance],
            device_id={"fs": self.place + step},
        )

    def z_arrival(self, index, way, distance):
        step = 1 if way == 0 else -1
        origin = self.place - step * distance
        target = self.gathered[index].at[origin, self.rows(index, self.half)]
        return pltpu.make_async_remote_copy(
            src_ref=target,
            dst_ref=target,
            send_sem=self.z_send.at[index, way, distance - 1],
            recv_sem=self.z_recv.at[index, way, distance - 1],
            device_id={"fs": self.place - step},
        )

    def y_copy(self, index, way, distance, incoming=False):
        step = 1 if way == 0 else -1
        origin = self.place - step * distance
        half = 1 - self.half if incoming else self.half
        target = self.gathered[index].at[origin, self.rows(index, half)]
        return pltpu.make_async_remote_copy(
            src_ref=target,
            dst_ref=target,
            send_sem=self.y_send.at[index, way, distance - 1],
            recv_sem=self.y_recv.at[index, way, distance - 1],
            device_id={"grp": 1 - self.half},
        )

    def own_copy(self, index):
        return pltpu.make_async_copy(
            self.sources[index], self.gathered[index].at[self.place], self.own_sem.at[index]
        )

    def start(self, index):
        for way in range(2):

            @pl.when(self.has(1 - 2 * way, 1))
            def _():
                self.z_copy(index, way, 0).start()

        self.own_copy(index).start()

    def relay(self, index, distance):
        for way in range(2):
            step = 1 - 2 * way

            @pl.when(self.has(-step, distance))
            def _():
                self.z_arrival(index, way, distance).wait_recv()
                if distance < self.count - 1:

                    @pl.when(self.has(step, 1))
                    def _():
                        self.z_copy(index, way, distance).start()

                self.y_copy(index, way, distance).start()

    def arrive(self, index):
        self.own_copy(index).wait()
        for distance in range(1, self.count):
            for way in range(2):

                @pl.when(self.has(2 * way - 1, distance))
                def _():
                    self.y_copy(index, way, distance, incoming=True).wait_recv()

    def drain(self, index):
        for distance in range(self.count):
            for way in range(2):
                step = 1 - 2 * way
                if distance < self.count - 1:

                    @pl.when(jnp.logical_and(self.has(-step, distance), self.has(step, 1)))
                    def _():
                        self.z_copy(index, way, distance).wait_send()

                if distance > 0:

                    @pl.when(self.has(-step, distance))
                    def _():
                        self.y_copy(index, way, distance).wait_send()


def gather_semaphores(weights, count):
    hops = pltpu.SemaphoreType.DMA((weights, 2, count - 1))
    return [hops, hops, hops, hops, pltpu.SemaphoreType.DMA((weights,))]


def gather_kernel(count, weights, *refs):
    gather = LineGather(count, refs[:weights], refs[weights : 2 * weights], refs[2 * weights :])
    gather.barrier()
    gather.start(0)
    for index in range(weights):
        if index + 1 < weights:
            gather.start(index + 1)
        for distance in range(1, count):
            gather.relay(index, distance)
    for index in range(weights):
        gather.arrive(index)
    for index in range(weights):
        gather.drain(index)


def gather_all(count, weights):
    return pl.pallas_call(
        functools.partial(gather_kernel, count, len(weights)),
        out_shape=[jax.ShapeDtypeStruct((count,) + w.shape, w.dtype) for w in weights],
        in_specs=[pl.BlockSpec(memory_space=pl.ANY)] * len(weights),
        out_specs=[pl.BlockSpec(memory_space=pltpu.VMEM)] * len(weights),
        scratch_shapes=gather_semaphores(len(weights), count),
        compiler_params=pltpu.CompilerParams(
            collective_id=0, has_side_effects=True, vmem_limit_bytes=60_000_000
        ),
    )(*weights)


def gather_plain(weights):
    return [lax.all_gather(w, "fs", axis=0, tiled=False) for w in weights]


def fits(mesh, weights):
    count = mesh.shape["fs"]
    return (
        mesh.shape["grp"] == 2
        and 2 <= count <= 4
        and all(w.shape[0] % 64 == 0 and w.shape[1] % 128 == 0 for w in weights)
        and count * sum(w.size for w in weights) <= 20_000_000
    )


def shards(
    mesh,
    tokens,
    mix_gain,
    val_weight,
    gate_weight,
    conv_taps,
    chan_gain,
    out_weight,
    mix_post_gain,
    ffn_gain,
    up_gate_weight,
    up_val_weight,
    ffn_taps,
    down_weight,
    ffn_post_gain,
):
    member = lax.axis_index("tp")
    weights = (val_weight, gate_weight, out_weight, up_gate_weight, up_val_weight, down_weight)
    if fits(mesh, weights):
        pieces = gather_all(mesh.shape["fs"], weights)
    else:
        pieces = gather_plain(weights)
    val_all, gate_all, gate_full, val_full = (
        pieces[i].reshape(-1, pieces[i].shape[2]) for i in (0, 1, 3, 4)
    )
    normed_own = rms_scale(tokens.astype(jnp.float32), mix_gain).astype(jnp.bfloat16)
    normed = lax.all_gather(normed_own, "tp", axis=0, tiled=True)
    local_ch = val_weight.shape[1]
    values, gate_sums = make_adder(
        normed,
        (
            val_all,
            gate_all,
        ),
    )
    glu_out = (values * jax.nn.sigmoid(gate_sums)).astype(jnp.bfloat16)
    own_taps = lax.dynamic_slice_in_dim(conv_taps, member * local_ch, local_ch, 1)
    conv_out = depthwise(glu_out, own_taps)
    totals, squares = lax.psum(
        (jnp.sum(conv_out, axis=1), jnp.sum(conv_out * conv_out, axis=1)), "tp"
    )
    all_channels = chan_gain.shape[0]
    chan_mean = totals[:, None] / all_channels
    chan_var = squares[:, None] / all_channels - chan_mean * chan_mean
    own_gain = lax.dynamic_slice_in_dim(chan_gain, member * local_ch, local_ch, 0).astype(
        jnp.float32
    )
    activated = jax.nn.silu((conv_out - chan_mean) * lax.rsqrt(chan_var + chan_epsilon) * own_gain)
    activated = activated.astype(jnp.bfloat16)
    out_full = jnp.concatenate(list(pieces[2]), axis=1)
    mixed_sum = lax.psum_scatter(
        make_rows_product(activated, out_full).astype(jnp.bfloat16),
        "tp",
        scatter_dimension=0,
        tiled=True,
    ).astype(jnp.float32)
    residual = (tokens.astype(jnp.float32) + rms_scale(mixed_sum, mix_post_gain)).astype(
        jnp.bfloat16
    )
    normed_share = rms_scale(residual.astype(jnp.float32), ffn_gain).astype(jnp.bfloat16)
    normed_ffn = lax.all_gather(normed_share, "tp", axis=0, tiled=True)
    local_ff = up_gate_weight.shape[1]
    own_ffn_taps = lax.dynamic_slice_in_dim(ffn_taps, member * local_ff, local_ff, 2)
    up_gate = jnp.dot(normed_ffn, gate_full, preferred_element_type=jnp.float32).astype(
        jnp.bfloat16
    )
    up_val = jnp.dot(normed_ffn, val_full, preferred_element_type=jnp.float32).astype(jnp.bfloat16)
    gate_conv = depthwise(up_gate, own_ffn_taps[0])
    val_conv = depthwise(up_val, own_ffn_taps[1])
    hidden = (jax.nn.gelu(gate_conv, approximate=True) * val_conv).astype(jnp.bfloat16)
    down_full = jnp.concatenate(list(pieces[5]), axis=1)
    ffn_sum = lax.psum_scatter(
        make_rows_product(hidden, down_full).astype(jnp.bfloat16),
        "tp",
        scatter_dimension=0,
        tiled=True,
    ).astype(jnp.float32)
    return (residual.astype(jnp.float32) + rms_scale(ffn_sum, ffn_post_gain)).astype(jnp.bfloat16)


def solution(mesh):
    return jax.shard_map(
        functools.partial(shards, mesh),
        mesh=mesh,
        in_specs=(
            P(("grp", "fs", "tp"), None),
            P(),
            P("fs", "tp"),
            P("fs", "tp"),
            P(),
            P(),
            P("tp", "fs"),
            P(),
            P(),
            P("fs", "tp"),
            P("fs", "tp"),
            P(),
            P("tp", "fs"),
            P(),
        ),
        out_specs=P(("grp", "fs", "tp"), None),
        check_vma=False,
    )
```

```python
import functools

import jax
import jax.numpy as jnp
from jax import lax
from jax.experimental import pallas as pl
from jax.experimental.pallas import tpu as pltpu
from jax.sharding import PartitionSpec as P

LEN = 64


norm_epsilon = 1e-06
chan_epsilon = 1e-05


def rms_scale(values, gain):
    inverse = lax.rsqrt(jnp.mean(values * values, axis=-1, keepdims=True) + norm_epsilon)
    return values * inverse * gain.astype(jnp.float32)


def depthwise(signal, tap_table):
    taps_count = tap_table.shape[0]
    channels = signal.shape[1]
    shaped = signal.astype(jnp.float32).reshape(signal.shape[0] // LEN, LEN, channels)
    padded = jnp.pad(shaped, ((0, 0), (taps_count - 1, 0), (0, 0)))
    tap_values = tap_table.astype(jnp.float32)
    result = jnp.zeros(shaped.shape, jnp.float32)
    for offset in range(taps_count):
        result = result + padded[:, offset : offset + LEN, :] * tap_values[offset]
    return result.reshape(signal.shape[0], channels)


def make_adder(left, pieces):
    first = jnp.dot(left, pieces[0], preferred_element_type=jnp.float32)
    second = jnp.dot(left, pieces[1], preferred_element_type=jnp.float32)
    return (first, second)


def make_rows_product(left, weight):
    return jnp.dot(left, weight, preferred_element_type=jnp.float32)


class LineGather:
    def __init__(self, count, chunks, sources, gathered, semaphores):
        self.chunks = chunks
        self.count = count
        self.sources = sources
        self.gathered = gathered
        self.z_send, self.z_recv, self.y_send, self.y_recv, self.own_sem = semaphores
        self.place = lax.axis_index("fs")
        self.half = lax.axis_index("grp")

    def barrier(self, extra=()):
        place, count = self.place, self.count
        semaphore = pltpu.get_barrier_semaphore()
        for step in (1, -1):

            @pl.when(self.has(step, 1))
            def _():
                pl.semaphore_signal(semaphore, inc=1, device_id={"fs": place + step})

        others = [{"grp": 1 - self.half}] + list(extra)
        for other in others:
            pl.semaphore_signal(semaphore, inc=1, device_id=other)
        inner = (place > 0).astype(jnp.int32) + (place < count - 1).astype(jnp.int32)
        pl.semaphore_wait(semaphore, inner + len(others))

    def has(self, step, distance):
        if step > 0:
            return self.place + distance < self.count
        return self.place >= distance

    def rows(self, index, half):
        weight, chunk = divmod(index, self.chunks)
        half_size = self.sources[weight].shape[0] // 2
        size = half_size // self.chunks
        return pl.ds(pl.multiple_of(half * half_size + chunk * size, size), size)

    def z_copy(self, index, way, distance):
        step = 1 if way == 0 else -1
        origin = self.place - step * distance
        rows = self.rows(index, self.half)
        target = self.gathered[index // self.chunks].at[origin, rows]
        source = self.sources[index // self.chunks].at[rows] if distance == 0 else target
        return pltpu.make_async_remote_copy(
            src_ref=source,
            dst_ref=target,
            send_sem=self.z_send.at[index, way, distance],
            recv_sem=self.z_recv.at[index, way, distance],
            device_id={"fs": self.place + step},
        )

    def z_arrival(self, index, way, distance):
        step = 1 if way == 0 else -1
        origin = self.place - step * distance
        target = self.gathered[index // self.chunks].at[origin, self.rows(index, self.half)]
        return pltpu.make_async_remote_copy(
            src_ref=target,
            dst_ref=target,
            send_sem=self.z_send.at[index, way, distance - 1],
            recv_sem=self.z_recv.at[index, way, distance - 1],
            device_id={"fs": self.place - step},
        )

    def y_copy(self, index, way, distance, incoming=False):
        step = 1 if way == 0 else -1
        origin = self.place - step * distance
        half = 1 - self.half if incoming else self.half
        target = self.gathered[index // self.chunks].at[origin, self.rows(index, half)]
        return pltpu.make_async_remote_copy(
            src_ref=target,
            dst_ref=target,
            send_sem=self.y_send.at[index, way, distance - 1],
            recv_sem=self.y_recv.at[index, way, distance - 1],
            device_id={"grp": 1 - self.half},
        )

    def own_copy(self, index):
        return pltpu.make_async_copy(
            self.sources[index], self.gathered[index].at[self.place], self.own_sem.at[index]
        )

    def start(self, index):
        for way in range(2):

            @pl.when(self.has(1 - 2 * way, 1))
            def _():
                self.z_copy(index, way, 0).start()

        if index % self.chunks == 0:
            self.own_copy(index // self.chunks).start()

    def relay(self, index, distance):
        for way in range(2):
            step = 1 - 2 * way

            @pl.when(self.has(-step, distance))
            def _():
                self.z_arrival(index, way, distance).wait_recv()
                if distance < self.count - 1:

                    @pl.when(self.has(step, 1))
                    def _():
                        self.z_copy(index, way, distance).start()

                self.y_copy(index, way, distance).start()

    def arrive(self, index):
        if index % self.chunks == 0:
            self.own_copy(index // self.chunks).wait()
        for distance in range(1, self.count):
            for way in range(2):

                @pl.when(self.has(2 * way - 1, distance))
                def _():
                    self.y_copy(index, way, distance, incoming=True).wait_recv()

    def drain(self, index):
        for distance in range(self.count):
            for way in range(2):
                step = 1 - 2 * way
                if distance < self.count - 1:

                    @pl.when(jnp.logical_and(self.has(-step, distance), self.has(step, 1)))
                    def _():
                        self.z_copy(index, way, distance).wait_send()

                if distance > 0:

                    @pl.when(self.has(-step, distance))
                    def _():
                        self.y_copy(index, way, distance).wait_send()


def gather_semaphores(weights, chunks, count):
    hops = pltpu.SemaphoreType.DMA((weights * chunks, 2, count - 1))
    return [hops, hops, hops, hops, pltpu.SemaphoreType.DMA((weights,))]


def gather_kernel(count, weights, chunks, *refs):
    gather = LineGather(
        count, chunks, refs[:weights], refs[weights : 2 * weights], refs[2 * weights :]
    )
    total = weights * chunks
    ahead = min(2, total)
    gather.barrier()
    for index in range(ahead):
        gather.start(index)
    for index in range(total):
        if index + ahead < total:
            gather.start(index + ahead)
        for distance in range(1, count):
            gather.relay(index, distance)
    for index in range(total):
        gather.arrive(index)
    for index in range(total):
        gather.drain(index)


def gather_all(mesh, weights, call, chunks, after):
    weights, after = lax.optimization_barrier((tuple(weights), after))
    if not fits(mesh, weights):
        return gather_plain(weights), after
    count = mesh.shape["fs"]
    held = sum(w.size * w.dtype.itemsize for w in weights)
    pieces = pl.pallas_call(
        functools.partial(gather_kernel, count, len(weights), chunks),
        out_shape=[jax.ShapeDtypeStruct((count,) + w.shape, w.dtype) for w in weights],
        in_specs=[pl.BlockSpec(memory_space=pl.ANY)] * len(weights),
        out_specs=[pl.BlockSpec(memory_space=pltpu.VMEM)] * len(weights),
        scratch_shapes=gather_semaphores(len(weights), chunks, count),
        cost_estimate=pl.CostEstimate(
            flops=0, bytes_accessed=held * 128, transcendentals=0
        ),
        compiler_params=pltpu.CompilerParams(
            collective_id=call, has_side_effects=True, vmem_limit_bytes=40_000_000
        ),
    )(*weights)
    return pieces, after


def gather_plain(weights):
    return [lax.all_gather(w, "fs", axis=0, tiled=False) for w in weights]


def fits(mesh, weights):
    count = mesh.shape["fs"]
    return (
        mesh.shape["grp"] == 2
        and 2 <= count <= 4
        and all(w.shape[0] % 128 == 0 and w.shape[1] % 128 == 0 for w in weights)
        and count * sum(w.size for w in weights) <= 20_000_000
    )


def shards(
    mesh,
    tokens,
    mix_gain,
    val_weight,
    gate_weight,
    conv_taps,
    chan_gain,
    out_weight,
    mix_post_gain,
    ffn_gain,
    up_gate_weight,
    up_val_weight,
    ffn_taps,
    down_weight,
    ffn_post_gain,
):
    member = lax.axis_index("tp")
    normed_own = rms_scale(tokens.astype(jnp.float32), mix_gain).astype(jnp.bfloat16)
    mix_pieces, normed_own = gather_all(
        mesh, (val_weight, gate_weight, out_weight), 0, 2, normed_own
    )
    val_all, gate_all = (p.reshape(-1, p.shape[2]) for p in mix_pieces[:2])
    normed = lax.all_gather(normed_own, "tp", axis=0, tiled=True)
    local_ch = val_weight.shape[1]
    values, gate_sums = make_adder(
        normed,
        (
            val_all,
            gate_all,
        ),
    )
    glu_out = (values * jax.nn.sigmoid(gate_sums)).astype(jnp.bfloat16)
    own_taps = lax.dynamic_slice_in_dim(conv_taps, member * local_ch, local_ch, 1)
    conv_out = depthwise(glu_out, own_taps)
    totals, squares = lax.psum(
        (jnp.sum(conv_out, axis=1), jnp.sum(conv_out * conv_out, axis=1)), "tp"
    )
    all_channels = chan_gain.shape[0]
    chan_mean = totals[:, None] / all_channels
    chan_var = squares[:, None] / all_channels - chan_mean * chan_mean
    own_gain = lax.dynamic_slice_in_dim(chan_gain, member * local_ch, local_ch, 0).astype(
        jnp.float32
    )
    activated = jax.nn.silu((conv_out - chan_mean) * lax.rsqrt(chan_var + chan_epsilon) * own_gain)
    activated = activated.astype(jnp.bfloat16)
    out_full = jnp.concatenate(list(mix_pieces[2]), axis=1)
    mix_part = make_rows_product(activated, out_full).astype(jnp.bfloat16)
    (gate_pieces,), mix_part = gather_all(mesh, (up_gate_weight,), 1, 4, mix_part)
    gate_full = gate_pieces.reshape(-1, gate_pieces.shape[2])
    mixed_sum = lax.psum_scatter(
        mix_part,
        "tp",
        scatter_dimension=0,
        tiled=True,
    ).astype(jnp.float32)
    residual = (tokens.astype(jnp.float32) + rms_scale(mixed_sum, mix_post_gain)).astype(
        jnp.bfloat16
    )
    normed_share = rms_scale(residual.astype(jnp.float32), ffn_gain).astype(jnp.bfloat16)
    (val_pieces,), normed_share = gather_all(mesh, (up_val_weight,), 2, 4, normed_share)
    val_full = val_pieces.reshape(-1, val_pieces.shape[2])
    normed_ffn = lax.all_gather(normed_share, "tp", axis=0, tiled=True)
    local_ff = up_gate_weight.shape[1]
    own_ffn_taps = lax.dynamic_slice_in_dim(ffn_taps, member * local_ff, local_ff, 2)
    up_gate = jnp.dot(normed_ffn, gate_full, preferred_element_type=jnp.float32).astype(
        jnp.bfloat16
    )
    up_val = jnp.dot(normed_ffn, val_full, preferred_element_type=jnp.float32).astype(jnp.bfloat16)
    gate_conv = depthwise(up_gate, own_ffn_taps[0])
    val_conv = depthwise(up_val, own_ffn_taps[1])
    hidden = (jax.nn.gelu(gate_conv, approximate=True) * val_conv).astype(jnp.bfloat16)
    (down_pieces,), hidden = gather_all(mesh, (down_weight,), 3, 4, hidden)
    down_full = jnp.concatenate(list(down_pieces), axis=1)
    ffn_sum = lax.psum_scatter(
        make_rows_product(hidden, down_full).astype(jnp.bfloat16),
        "tp",
        scatter_dimension=0,
        tiled=True,
    ).astype(jnp.float32)
    return (residual.astype(jnp.float32) + rms_scale(ffn_sum, ffn_post_gain)).astype(jnp.bfloat16)


def solution(mesh):
    return jax.shard_map(
        functools.partial(shards, mesh),
        mesh=mesh,
        in_specs=(
            P(("grp", "fs", "tp"), None),
            P(),
            P("fs", "tp"),
            P("fs", "tp"),
            P(),
            P(),
            P("tp", "fs"),
            P(),
            P(),
            P("fs", "tp"),
            P("fs", "tp"),
            P(),
            P("tp", "fs"),
            P(),
        ),
        out_specs=P(("grp", "fs", "tp"), None),
        check_vma=False,
    )
```

```python
import functools

import jax
import jax.numpy as jnp
from jax import lax
from jax.experimental import pallas as pl
from jax.experimental.pallas import tpu as pltpu
from jax.sharding import PartitionSpec as P

LEN = 64


norm_epsilon = 1e-06
chan_epsilon = 1e-05


def rms_scale(values, gain):
    inverse = lax.rsqrt(jnp.mean(values * values, axis=-1, keepdims=True) + norm_epsilon)
    return values * inverse * gain.astype(jnp.float32)


def depthwise(signal, tap_table):
    taps_count = tap_table.shape[0]
    channels = signal.shape[1]
    shaped = signal.astype(jnp.float32).reshape(signal.shape[0] // LEN, LEN, channels)
    padded = jnp.pad(shaped, ((0, 0), (taps_count - 1, 0), (0, 0)))
    tap_values = tap_table.astype(jnp.float32)
    result = jnp.zeros(shaped.shape, jnp.float32)
    for offset in range(taps_count):
        result = result + padded[:, offset : offset + LEN, :] * tap_values[offset]
    return result.reshape(signal.shape[0], channels)


def make_adder(left, pieces):
    first = jnp.dot(left, pieces[0], preferred_element_type=jnp.float32)
    second = jnp.dot(left, pieces[1], preferred_element_type=jnp.float32)
    return (first, second)


def make_rows_product(left, weight):
    return jnp.dot(left, weight, preferred_element_type=jnp.float32)


class LineGather:
    def __init__(self, count, chunks, sources, gathered, semaphores):
        self.chunks = chunks
        self.count = count
        self.sources = sources
        self.gathered = gathered
        self.z_send, self.z_recv, self.y_send, self.y_recv, self.own_sem = semaphores
        self.place = lax.axis_index("fs")
        self.half = lax.axis_index("grp")

    def barrier(self, extra=()):
        place, count = self.place, self.count
        semaphore = pltpu.get_barrier_semaphore()
        for step in (1, -1):

            @pl.when(self.has(step, 1))
            def _():
                pl.semaphore_signal(semaphore, inc=1, device_id={"fs": place + step})

        others = [{"grp": 1 - self.half}] + list(extra)
        for other in others:
            pl.semaphore_signal(semaphore, inc=1, device_id=other)
        inner = (place > 0).astype(jnp.int32) + (place < count - 1).astype(jnp.int32)
        pl.semaphore_wait(semaphore, inner + len(others))

    def has(self, step, distance):
        if step > 0:
            return self.place + distance < self.count
        return self.place >= distance

    def rows(self, index, half):
        weight, chunk = divmod(index, self.chunks)
        half_size = self.sources[weight].shape[0] // 2
        size = half_size // self.chunks
        return pl.ds(pl.multiple_of(half * half_size + chunk * size, size), size)

    def z_copy(self, index, way, distance):
        step = 1 if way == 0 else -1
        origin = self.place - step * distance
        rows = self.rows(index, self.half)
        target = self.gathered[index // self.chunks].at[origin, rows]
        source = self.sources[index // self.chunks].at[rows] if distance == 0 else target
        return pltpu.make_async_remote_copy(
            src_ref=source,
            dst_ref=target,
            send_sem=self.z_send.at[index, way, distance],
            recv_sem=self.z_recv.at[index, way, distance],
            device_id={"fs": self.place + step},
        )

    def z_arrival(self, index, way, distance):
        step = 1 if way == 0 else -1
        origin = self.place - step * distance
        target = self.gathered[index // self.chunks].at[origin, self.rows(index, self.half)]
        return pltpu.make_async_remote_copy(
            src_ref=target,
            dst_ref=target,
            send_sem=self.z_send.at[index, way, distance - 1],
            recv_sem=self.z_recv.at[index, way, distance - 1],
            device_id={"fs": self.place - step},
        )

    def y_copy(self, index, way, distance, incoming=False):
        step = 1 if way == 0 else -1
        origin = self.place - step * distance
        half = 1 - self.half if incoming else self.half
        target = self.gathered[index // self.chunks].at[origin, self.rows(index, half)]
        return pltpu.make_async_remote_copy(
            src_ref=target,
            dst_ref=target,
            send_sem=self.y_send.at[index, way, distance - 1],
            recv_sem=self.y_recv.at[index, way, distance - 1],
            device_id={"grp": 1 - self.half},
        )

    def own_copy(self, index):
        return pltpu.make_async_copy(
            self.sources[index], self.gathered[index].at[self.place], self.own_sem.at[index]
        )

    def start(self, index):
        for way in range(2):

            @pl.when(self.has(1 - 2 * way, 1))
            def _():
                self.z_copy(index, way, 0).start()

        if index % self.chunks == 0:
            self.own_copy(index // self.chunks).start()

    def relay(self, index, distance):
        for way in range(2):
            step = 1 - 2 * way

            @pl.when(self.has(-step, distance))
            def _():
                self.z_arrival(index, way, distance).wait_recv()
                if distance < self.count - 1:

                    @pl.when(self.has(step, 1))
                    def _():
                        self.z_copy(index, way, distance).start()

                self.y_copy(index, way, distance).start()

    def arrive(self, index):
        if index % self.chunks == 0:
            self.own_copy(index // self.chunks).wait()
        for distance in range(1, self.count):
            for way in range(2):

                @pl.when(self.has(2 * way - 1, distance))
                def _():
                    self.y_copy(index, way, distance, incoming=True).wait_recv()

    def drain(self, index):
        for distance in range(self.count):
            for way in range(2):
                step = 1 - 2 * way
                if distance < self.count - 1:

                    @pl.when(jnp.logical_and(self.has(-step, distance), self.has(step, 1)))
                    def _():
                        self.z_copy(index, way, distance).wait_send()

                if distance > 0:

                    @pl.when(self.has(-step, distance))
                    def _():
                        self.y_copy(index, way, distance).wait_send()


def gather_semaphores(weights, chunks, count):
    hops = pltpu.SemaphoreType.DMA((weights * chunks, 2, count - 1))
    return [hops, hops, hops, hops, pltpu.SemaphoreType.DMA((weights,))]


def gather_kernel(count, weights, chunks, *refs):
    gather = LineGather(
        count, chunks, refs[:weights], refs[weights : 2 * weights], refs[2 * weights :]
    )
    total = weights * chunks
    ahead = min(2, total)
    gather.barrier()
    for index in range(ahead):
        gather.start(index)
    for index in range(total):
        if index + ahead < total:
            gather.start(index + ahead)
        for distance in range(1, count):
            gather.relay(index, distance)
    for index in range(total):
        gather.arrive(index)
    for index in range(total):
        gather.drain(index)


def gather_all(mesh, weights, call, chunks, after):
    weights, after = lax.optimization_barrier((tuple(weights), after))
    if not fits(mesh, weights):
        return gather_plain(weights), after
    count = mesh.shape["fs"]
    held = sum(w.size * w.dtype.itemsize for w in weights)
    pieces = pl.pallas_call(
        functools.partial(gather_kernel, count, len(weights), chunks),
        out_shape=[jax.ShapeDtypeStruct((count,) + w.shape, w.dtype) for w in weights],
        in_specs=[pl.BlockSpec(memory_space=pl.ANY)] * len(weights),
        out_specs=[pl.BlockSpec(memory_space=pltpu.VMEM)] * len(weights),
        scratch_shapes=gather_semaphores(len(weights), chunks, count),
        cost_estimate=pl.CostEstimate(
            flops=0, bytes_accessed=held * 128, transcendentals=0
        ),
        compiler_params=pltpu.CompilerParams(
            collective_id=call, has_side_effects=True, vmem_limit_bytes=40_000_000
        ),
    )(*weights)
    return pieces, after


def gather_plain(weights):
    return [lax.all_gather(w, "fs", axis=0, tiled=False) for w in weights]


def fits(mesh, weights):
    count = mesh.shape["fs"]
    return (
        mesh.shape["grp"] == 2
        and 2 <= count <= 4
        and all(w.shape[0] % 128 == 0 and w.shape[1] % 128 == 0 for w in weights)
        and count * sum(w.size for w in weights) <= 20_000_000
    )


def shards(
    mesh,
    tokens,
    mix_gain,
    val_weight,
    gate_weight,
    conv_taps,
    chan_gain,
    out_weight,
    mix_post_gain,
    ffn_gain,
    up_gate_weight,
    up_val_weight,
    ffn_taps,
    down_weight,
    ffn_post_gain,
):
    member = lax.axis_index("tp")
    normed_own = rms_scale(tokens.astype(jnp.float32), mix_gain).astype(jnp.bfloat16)
    mix_pieces, normed_own = gather_all(
        mesh, (val_weight, gate_weight, out_weight), 0, 2, normed_own
    )
    val_all, gate_all = (p.reshape(-1, p.shape[2]) for p in mix_pieces[:2])
    normed = lax.all_gather(normed_own, "tp", axis=0, tiled=True)
    local_ch = val_weight.shape[1]
    values, gate_sums = make_adder(
        normed,
        (
            val_all,
            gate_all,
        ),
    )
    glu_out = (values * jax.nn.sigmoid(gate_sums)).astype(jnp.bfloat16)
    own_taps = lax.dynamic_slice_in_dim(conv_taps, member * local_ch, local_ch, 1)
    conv_out = depthwise(glu_out, own_taps)
    totals, squares = lax.psum(
        (jnp.sum(conv_out, axis=1), jnp.sum(conv_out * conv_out, axis=1)), "tp"
    )
    all_channels = chan_gain.shape[0]
    chan_mean = totals[:, None] / all_channels
    chan_var = squares[:, None] / all_channels - chan_mean * chan_mean
    own_gain = lax.dynamic_slice_in_dim(chan_gain, member * local_ch, local_ch, 0).astype(
        jnp.float32
    )
    activated = jax.nn.silu((conv_out - chan_mean) * lax.rsqrt(chan_var + chan_epsilon) * own_gain)
    activated = activated.astype(jnp.bfloat16)
    out_full = jnp.concatenate(list(mix_pieces[2]), axis=1)
    mix_part = make_rows_product(activated, out_full).astype(jnp.bfloat16)
    up_weights = (up_gate_weight, up_val_weight)
    (gate_pieces, val_pieces), mix_part = gather_all(mesh, up_weights, 1, 4, mix_part)
    gate_full = gate_pieces.reshape(-1, gate_pieces.shape[2])
    mixed_sum = lax.psum_scatter(mix_part, "tp", scatter_dimension=0, tiled=True)
    mixed_sum = mixed_sum.astype(jnp.float32)
    residual = (tokens.astype(jnp.float32) + rms_scale(mixed_sum, mix_post_gain)).astype(
        jnp.bfloat16
    )
    normed_share = rms_scale(residual.astype(jnp.float32), ffn_gain).astype(jnp.bfloat16)
    (down_pieces,), normed_share = gather_all(mesh, (down_weight,), 2, 4, normed_share)
    val_full = val_pieces.reshape(-1, val_pieces.shape[2])
    normed_ffn = lax.all_gather(normed_share, "tp", axis=0, tiled=True)
    local_ff = up_gate_weight.shape[1]
    own_ffn_taps = lax.dynamic_slice_in_dim(ffn_taps, member * local_ff, local_ff, 2)
    up_gate = jnp.dot(normed_ffn, gate_full, preferred_element_type=jnp.float32).astype(
        jnp.bfloat16
    )
    up_val = jnp.dot(normed_ffn, val_full, preferred_element_type=jnp.float32).astype(jnp.bfloat16)
    gate_conv = depthwise(up_gate, own_ffn_taps[0])
    val_conv = depthwise(up_val, own_ffn_taps[1])
    hidden = (jax.nn.gelu(gate_conv, approximate=True) * val_conv).astype(jnp.bfloat16)
    down_full = jnp.concatenate(list(down_pieces), axis=1)
    ffn_sum = lax.psum_scatter(
        make_rows_product(hidden, down_full).astype(jnp.bfloat16),
        "tp",
        scatter_dimension=0,
        tiled=True,
    ).astype(jnp.float32)
    return (residual.astype(jnp.float32) + rms_scale(ffn_sum, ffn_post_gain)).astype(jnp.bfloat16)


def solution(mesh):
    return jax.shard_map(
        functools.partial(shards, mesh),
        mesh=mesh,
        in_specs=(
            P(("grp", "fs", "tp"), None),
            P(),
            P("fs", "tp"),
            P("fs", "tp"),
            P(),
            P(),
            P("tp", "fs"),
            P(),
            P(),
            P("fs", "tp"),
            P("fs", "tp"),
            P(),
            P("tp", "fs"),
            P(),
        ),
        out_specs=P(("grp", "fs", "tp"), None),
        check_vma=False,
    )
```
